32 devices in a mesh: grp: 2 (over y), fs: 8 (over z, core), tp: 2 (over x).
Axes of the slice: x: 2, y: 2, z: 4, core: 2. Of those that a mesh axis runs over, the one named last changes fastest.
Arguments:
- prompt: bfloat16 [6144, 2048], P(('grp', 'fs')), parts along dimension 0, may hold values from -6 to 6
- routes: int32 [6144, 4], P(('grp', 'fs')), parts along dimension 0, may hold values from 0 to 7, all different within a row; in each aligned block of 384 rows (0 to 383, 384 to 767, ...) at most 240 rows name the same one
- route_weight: float32 [6144, 4], P(('grp', 'fs')), parts along dimension 0, may hold values from 0.2 to 1
- norm_gain: float32 [2048], P('fs'), may hold values from 0.1 to 1.9
- gate_train: float32 [8, 2048, 1024], P(None, 'fs', 'tp'), may hold values from -0.4 to 0.4
- up_train: float32 [8, 2048, 1024], P(None, 'fs', 'tp'), may hold values from -0.4 to 0.4
- down_train: float32 [8, 1024, 2048], P(None, 'fs', 'tp'), may hold values from -0.07 to 0.07
Outputs:
- gate_serve: bfloat16 [16, 2048, 1024], P(('grp', 'fs'), None, 'tp'), parts along dimension 0
- up_serve: bfloat16 [16, 2048, 1024], P(('grp', 'fs'), None, 'tp'), parts along dimension 0
- down_serve: bfloat16 [16, 1024, 2048], P(('grp', 'fs'), 'tp'), parts along dimension 0
- mixed: bfloat16 [6144, 2048], P(('grp', 'fs'), 'tp'), parts along dimension 0
The draws below stay inside these ranges and needn't reach their ends.
There are 2 independent parts, one for each index of `grp`. The reference program is written for one: setup_inputs(seed, part) draws one part's arguments, and reference() takes and returns one part's arrays. A program takes and returns all parts, laid end to end along the dimension named above; an argument that names none is the same for every part. Nothing has to cross between parts.
Inputs may be any that keep to these rules, and one draw needn't show every extreme that they name: `routes`: each row names 4 different experts. Among the rows of one index of fs no expert is named more than 240 times, a bound that some block reaches on some index.
All inputs are finite; a program needn't handle non-finite values.
Results may differ from the reference program's by a relative error of at most 0.012.
Values may be sent and summed in bfloat16 or wider, within the bound.
No kernel may reach another device: no remote copies, remote signals or barrier semaphores. Data moves between devices by JAX's collectives and lax.ppermute only.
A program may use at most 128 MiB of HBM per device.

```python
import math
import jax
import jax.numpy as jnp
import numpy as np
from jax import lax

D = 2048
FF = 1024
TOP = 4
TOK_DEV = 384
EXPERTS = 8
CAP = 240
TOKENS = 3072
N_FS = 8
N_TP = 2


def shard_levels(stream_key, extent, shards, least, top_value):
    loudness, own = 1.0, jax.random.fold_in(stream_key, 6)
    for dim, parts in shards:
        heights = jnp.exp(jax.random.uniform(jax.random.fold_in(own, dim), (parts,), jnp.float32, least / len(shards), top_value / len(shards)))
        loudness = loudness * jnp.repeat(heights, extent[dim] // parts).reshape([-1 if axis == dim else 1 for axis in range(len(extent))])
    return loudness


def deal_out(own_key, own, number, rows, number_of, top, reach, slope):
    sequence = jax.random.permutation(own_key, number_of)
    packed, common = portions_of(number_of, rows * top, reach, slope, True), portions_of(number_of, rows * top, reach, slope, False)
    places = jnp.arange(number_of)

    def named(lengths, turn):
        used = int((lengths > 0).sum())
        fixed = max(1, used // 4)
        passed = fixed + (places - fixed + turn * (used - fixed)) % max(1, number_of - fixed)
        return jnp.zeros((number_of,), jnp.int32).at[sequence[jnp.where(places < fixed, places, passed)]].set(jnp.asarray(lengths, jnp.int32))

    lengths = jnp.where(number % 4 == 0, named(packed, number // 4), named(common, number - number // 4 - 1))
    mixed = jax.random.permutation(jax.random.fold_in(own, 3), number_of)
    donor, receiver = mixed[0:number_of // 2 * 2:2], mixed[1:number_of // 2 * 2:2]
    slack = jnp.minimum(lengths[donor] - 1, reach - lengths[receiver]) // 2
    slack = jnp.where((donor == sequence[0]) | (receiver == sequence[0]) | (lengths[receiver] == 0), 0, jnp.maximum(slack, 0))
    passed = jax.random.randint(jax.random.fold_in(own, 4), (number_of // 2,), 0, 1 << 20) % (slack + 1)
    lengths = lengths.at[donor].add(-passed).at[receiver].add(passed)
    members = jnp.searchsorted(jnp.cumsum(lengths), jnp.arange(rows * top), side="right").astype(jnp.int32)
    grid = members.reshape(top, rows).T
    grid = grid[jax.random.permutation(jax.random.fold_in(own, 1), rows)]
    turn = jax.random.randint(jax.random.fold_in(own, 2), (rows, 1), 0, top)
    return jnp.take_along_axis(grid, (jnp.arange(top)[None, :] + turn) % top, axis=1)


def portions_of(count, total, limit, slope, full):
    portions = [(1 << 20) // math.isqrt(rank ** slope) + 1 for rank in range(1, count + 1)]
    largest = limit if full else min(limit, max(-(-total // count), total * portions[0] // sum(portions)))
    least = 1 if total - largest >= count - 1 else 0
    counts, rest = [largest] + [least] * (count - 1), total - largest - least * (count - 1)
    while rest > 0:
        candidates = [i for i in range(1, count) if counts[i] < largest] or [i for i in range(1, count) if counts[i] < limit]
        mass, budget = sum([portions[i] for i in candidates]), rest
        for i in candidates:
            more = min(limit - counts[i], max(1, budget * portions[i] // mass), rest)
            counts[i] = counts[i] + more
            rest = rest - more
    return np.array(counts)


def scatter_about(rng, dims, scale, limit, cuts=(), held_as=jnp.bfloat16):
    values = jax.random.normal(rng, dims, jnp.float32) * scale
    if len(cuts) > 0:
        values = shard_levels(rng, dims, cuts, -0.22, 0.18) * values
    return jnp.clip(values, min=-limit, max=limit).astype(held_as)


def setup_inputs(seed: int = 0, part: int = 0) -> dict:
    keys = jax.random.split(jax.random.key(seed), 8)
    part_splits = jax.random.split(jax.random.fold_in(keys[7], part), 8)
    prompt = scatter_about(part_splits[0], (TOKENS, D), 1.0, 6.0, ((0, 8),))
    routes_keys = jax.random.split(jax.random.fold_in(part_splits[1], 1), TOKENS // TOK_DEV)
    routes_turns = jax.random.permutation(jax.random.fold_in(part_splits[1], 3), TOKENS // TOK_DEV)
    routes = jax.vmap(lambda own, number: deal_out(jax.random.fold_in(part_splits[1], 2), own, number, TOK_DEV, EXPERTS, TOP, CAP, 1))(routes_keys, routes_turns).reshape((TOKENS, TOP))
    route_weight = jnp.clip(jnp.exp(math.log(1.0) - 1.609438 * jax.random.uniform(part_splits[2], (TOKENS, TOP), jnp.float32) ** shard_levels(part_splits[2], (TOKENS, TOP), ((0, 8),), -0.2, 0.2)), 0.2, 1.0)
    norm_gain = jnp.clip(1.0 + 0.18 * jax.random.normal(keys[3], (D,), jnp.float32), 0.1, 1.9)
    gate_train = scatter_about(keys[4], (EXPERTS, D, FF), 0.055, 0.4, ((1, 8), (2, 2)), jnp.float32)
    up_train = scatter_about(keys[5], (EXPERTS, D, FF), 0.055, 0.4, ((1, 8), (2, 2)), jnp.float32)
    down_train = scatter_about(keys[6], (EXPERTS, FF, D), 0.01, 0.07, ((1, 8), (2, 2)), jnp.float32)
    return {"prompt": prompt, "routes": routes, "route_weight": route_weight, "norm_gain": norm_gain, "gate_train": gate_train, "up_train": up_train, "down_train": down_train}


LIMIT = 7.0
ALPHA = 1.702
EPS = 1e-06

def expert_apply(rows, gate_one, up_one, down_one):
    gate_pre = jnp.dot(rows, gate_one, preferred_element_type=jnp.float32)
    up_pre = jnp.dot(rows, up_one, preferred_element_type=jnp.float32)
    gate_pre = jnp.minimum(gate_pre, LIMIT)
    up_pre = jnp.clip(up_pre, -LIMIT, LIMIT)
    hidden = ((up_pre + 1.0) * gate_pre * jax.nn.sigmoid(ALPHA * gate_pre)).astype(jnp.bfloat16)
    width = hidden.shape[1] // N_TP
    total = jnp.zeros((rows.shape[0], down_one.shape[1]), jnp.float32)
    for block in range(N_TP):
        part = jnp.dot(hidden[:, block * width:(block + 1) * width], down_one[block * width:(block + 1) * width], preferred_element_type=jnp.float32).astype(jnp.bfloat16)
        part = lax.optimization_barrier(part)
        total = total + part.astype(jnp.float32)
    return total.astype(jnp.bfloat16)

def reference(prompt, routes, route_weight, norm_gain, gate_train, up_train, down_train):
    gate_serve = (norm_gain[None, :, None] * gate_train).astype(jnp.bfloat16)
    up_serve = (norm_gain[None, :, None] * up_train).astype(jnp.bfloat16)
    down_serve = down_train.astype(jnp.bfloat16)
    values = prompt.astype(jnp.float32)
    normed = (values * lax.rsqrt(lax.optimization_barrier(jnp.mean(values * values, axis=-1, keepdims=True)) + EPS)).astype(jnp.bfloat16)
    flat_expert = routes.reshape(-1).astype(jnp.int32)
    flat_weight = route_weight.reshape(-1)
    most = N_FS * CAP
    experts = gate_serve.shape[0]

    def one_expert(carry, expert):
        chosen = flat_expert == expert
        picks = jnp.nonzero(chosen, size=most, fill_value=0)[0].astype(jnp.int32)
        live = jnp.arange(most, dtype=jnp.int32) < jnp.sum(chosen.astype(jnp.int32))
        token = (picks // TOP).astype(jnp.int32)
        rows = normed[token]
        result = expert_apply(rows, gate_serve[expert], up_serve[expert], down_serve[expert])
        scale = jnp.where(live, flat_weight[picks], 0.0).astype(jnp.float32)
        carry = carry.at[token].add(result.astype(jnp.float32) * scale[:, None])
        return (carry, None)
    start = jnp.zeros(normed.shape, jnp.float32)
    total, unused = lax.scan(one_expert, start, jnp.arange(experts, dtype=jnp.int32))
    return (gate_serve, up_serve, down_serve, total.astype(jnp.bfloat16))
```

```python
import jax
import jax.numpy as jnp
from jax import lax
from jax.sharding import PartitionSpec as P

LIMIT = 7.0
ALPHA = 1.702
EPS = 1e-06


def ring_pieces(send_block, axis):
    size = lax.axis_size(axis)
    pieces = [send_block(0)]
    for step in range(1, size):
        perm = [(src, (src + step) % size) for src in range(size)]
        pieces.append(lax.ppermute(send_block(step), axis, perm))
    return pieces


def by_source(pieces, axis):
    size = len(pieces)
    me = lax.axis_index(axis)
    ordered = []
    for source in range(size):
        step = (me - source) % size
        out = pieces[0]
        for index in range(1, size):
            out = jnp.where(step == index, pieces[index], out)
        ordered.append(out)
    return ordered


def shards(prompt, routes, route_weight, norm_gain, gate_train, up_train, down_train):
    grp, fs, tp = (lax.axis_size(name) for name in ("grp", "fs", "tp"))
    my_grp, my_tp = lax.axis_index("grp"), lax.axis_index("tp")
    tok_rows, width = prompt.shape
    top = routes.shape[1]
    experts, d_rows, own_width = gate_train.shape
    f_rows, out_cols = down_train.shape[1:]
    capacity = min(tok_rows, max(2, 5 * tok_rows * top // (4 * experts)))

    chosen = routes[None, :, :] == jnp.arange(experts, dtype=jnp.int32)[:, None, None]
    table = jnp.sum(jnp.where(chosen, route_weight[None, :, :], 0.0), axis=2)
    weight = lax.all_to_all(table, "fs", split_axis=0, concat_axis=0, tiled=True)
    values = prompt.astype(jnp.float32)
    normed = (values * lax.rsqrt(jnp.mean(values * values, axis=-1, keepdims=True) + EPS)).astype(
        jnp.bfloat16
    )
    tokens = lax.all_gather(normed, "fs", axis=0, tiled=False)

    share = d_rows // grp
    gain = norm_gain[None, :, None]
    start = my_grp * share
    gate_part = lax.dynamic_slice_in_dim(gate_train, start, share, 1)
    up_part = lax.dynamic_slice_in_dim(up_train, start, share, 1)
    gain_part = lax.dynamic_slice_in_dim(gain, start, share, 1)
    both = jnp.concatenate([gain_part * gate_part, gain_part * up_part], axis=1).astype(jnp.bfloat16)
    both = lax.all_to_all(both, "fs", split_axis=0, concat_axis=0, tiled=True)
    both = by_source(ring_pieces(lambda step: both, "grp"), "grp")
    gate_mine, up_mine = (
        jnp.stack([piece[:, at : at + share] for piece in both], axis=1).reshape(
            fs * d_rows, own_width
        )
        for at in (0, share)
    )
    f_share = f_rows // grp
    down_part = lax.dynamic_slice_in_dim(down_train, my_grp * f_share, f_share, 1).astype(
        jnp.bfloat16
    )
    down_part = lax.all_to_all(down_part, "fs", split_axis=0, concat_axis=0, tiled=True)
    down_part = by_source(ring_pieces(lambda step: down_part, "grp"), "grp")
    down_rows = jnp.stack(down_part, axis=1).reshape(fs * f_rows, out_cols)

    def down_block(step):
        return lax.dynamic_slice_in_dim(
            down_rows, ((my_tp + step) % tp) * own_width, own_width, 0
        )

    down_mine = jnp.concatenate(by_source(ring_pieces(down_block, "tp"), "tp"), axis=1)

    mask = weight > 0.0
    flags = mask.astype(jnp.bfloat16)
    order = jnp.arange(tok_rows, dtype=jnp.int32)
    before = (order[:, None] < order[None, :]).astype(jnp.bfloat16)
    place = jnp.dot(flags, before, preferred_element_type=jnp.float32).astype(jnp.int32)
    slots = jnp.arange(capacity, dtype=jnp.int32)
    pick = ((place[:, None, :] == slots[None, :, None]) & mask[:, None, :]).astype(jnp.bfloat16)
    inbox = (
        jnp.einsum("sct,std->scd", pick, tokens, preferred_element_type=jnp.float32)
        .astype(jnp.bfloat16)
        .reshape(fs * capacity, width)
    )
    gate_pre = jnp.dot(inbox, gate_mine, preferred_element_type=jnp.float32)
    up_pre = jnp.dot(inbox, up_mine, preferred_element_type=jnp.float32)
    gate_pre = jnp.minimum(gate_pre, LIMIT)
    up_pre = jnp.clip(up_pre, -LIMIT, LIMIT)
    hidden = ((up_pre + 1.0) * gate_pre * jax.nn.sigmoid(ALPHA * gate_pre)).astype(jnp.bfloat16)
    total = 0.0
    for step, cols in enumerate(ring_pieces(lambda step: hidden, "tp")):
        total = total + jnp.dot(cols, down_block(-step), preferred_element_type=jnp.float32)
    summed = total.astype(jnp.bfloat16).reshape(fs, capacity, out_cols)
    back = jnp.einsum("sct,scd->std", pick, summed, preferred_element_type=jnp.float32)
    back = (back * weight[:, :, None]).astype(jnp.bfloat16).reshape(fs * tok_rows, out_cols)
    mixed = lax.psum_scatter(back, "fs", scatter_dimension=0, tiled=True)
    return (gate_mine[None], up_mine[None], down_mine[None], mixed)


def solution(mesh):
    return jax.shard_map(
        shards,
        mesh=mesh,
        in_specs=(
            P(("grp", "fs"), None),
            P(("grp", "fs"), None),
            P(("grp", "fs"), None),
            P("fs"),
            P(None, "fs", "tp"),
            P(None, "fs", "tp"),
            P(None, "fs", "tp"),
        ),
        out_specs=(
            P(("grp", "fs"), None, "tp"),
            P(("grp", "fs"), None, "tp"),
            P(("grp", "fs"), "tp", None),
            P(("grp", "fs"), "tp"),
        ),
        check_vma=False,
    )
```

```python
import jax
import jax.numpy as jnp
from jax import lax
from jax.sharding import PartitionSpec as P

LIMIT = 7.0
ALPHA = 1.702
EPS = 1e-06
CHUNKS = 2


def ring_pieces(send_block, axis):
    size = lax.axis_size(axis)
    pieces = [send_block(0)]
    for step in range(1, size):
        perm = [(src, (src + step) % size) for src in range(size)]
        pieces.append(lax.ppermute(send_block(step), axis, perm))
    return pieces


def by_source(pieces, axis):
    size = len(pieces)
    me = lax.axis_index(axis)
    ordered = []
    for source in range(size):
        step = (me - source) % size
        out = pieces[0]
        for index in range(1, size):
            out = jnp.where(step == index, pieces[index], out)
        ordered.append(out)
    return ordered


def shards(prompt, routes, route_weight, norm_gain, gate_train, up_train, down_train):
    grp, fs, tp = (lax.axis_size(name) for name in ("grp", "fs", "tp"))
    my_grp, my_tp = lax.axis_index("grp"), lax.axis_index("tp")
    tok_rows, width = prompt.shape
    top = routes.shape[1]
    experts, d_rows, own_width = gate_train.shape
    f_rows, out_cols = down_train.shape[1:]
    capacity = min(tok_rows, max(2, 5 * tok_rows * top // (4 * experts)))

    chosen = routes[None, :, :] == jnp.arange(experts, dtype=jnp.int32)[:, None, None]
    table = jnp.sum(jnp.where(chosen, route_weight[None, :, :], 0.0), axis=2)
    weight = lax.all_to_all(table, "fs", split_axis=0, concat_axis=0, tiled=True)
    values = prompt.astype(jnp.float32)
    normed = (values * lax.rsqrt(jnp.mean(values * values, axis=-1, keepdims=True) + EPS)).astype(
        jnp.bfloat16
    )
    near = width // 2
    near_share = near // tp
    near_tokens = lax.all_gather(
        lax.dynamic_slice_in_dim(normed, my_tp * near_share, near_share, 1), "fs", axis=0, tiled=False
    )

    share = d_rows // grp
    gain_part = lax.dynamic_slice_in_dim(norm_gain, my_grp * share, share, 0)[None, :, None]

    def served(mine, rows):
        pieces = by_source(ring_pieces(lambda step: mine, "grp"), "grp")
        return jnp.stack(pieces, axis=1).reshape(fs * rows, mine.shape[2])

    def scaled(train):
        part = lax.dynamic_slice_in_dim(train, my_grp * share, share, 1)
        return (gain_part * part).astype(jnp.bfloat16)

    def over_fs(part):
        return lax.all_to_all(part, "fs", split_axis=0, concat_axis=0, tiled=True)

    gate_part = over_fs(scaled(gate_train))
    up_part = scaled(up_train)
    gate_part, up_part = lax.optimization_barrier((gate_part, up_part))
    up_part = over_fs(up_part)
    far, up_part = lax.optimization_barrier((normed[:, near:], up_part))
    far_tokens = lax.all_gather(far, "fs", axis=0, tiled=False)
    gate_mine = served(gate_part, d_rows)
    up_mine = served(up_part, d_rows)
    f_share = f_rows // grp
    down_part = lax.dynamic_slice_in_dim(down_train, my_grp * f_share, f_share, 1).astype(
        jnp.bfloat16
    )
    far_tokens, down_part = lax.optimization_barrier((far_tokens, down_part))
    down_rows = served(over_fs(down_part), f_rows)

    def down_block(step):
        return lax.dynamic_slice_in_dim(
            down_rows, ((my_tp + step) % tp) * own_width, own_width, 0
        )

    down_mine = jnp.concatenate(by_source(ring_pieces(down_block, "tp"), "tp"), axis=1)

    mask = weight > 0.0
    flags = mask.astype(jnp.bfloat16)
    order = jnp.arange(tok_rows, dtype=jnp.int32)
    before = (order[:, None] < order[None, :]).astype(jnp.bfloat16)
    place = jnp.dot(flags, before, preferred_element_type=jnp.float32).astype(jnp.int32)
    slots = jnp.arange(capacity, dtype=jnp.int32)
    pick = ((place[:, None, :] == slots[None, :, None]) & mask[:, None, :]).astype(jnp.bfloat16)

    def compact(rows, part):
        picked = jnp.einsum("sct,std->scd", part, rows, preferred_element_type=jnp.float32)
        return picked.astype(jnp.bfloat16).reshape(-1, rows.shape[2])

    near_rows = compact(near_tokens, pick)
    near_rows = ring_pieces(lambda step: near_rows, "tp")
    chunk = fs // CHUNKS
    outs = []
    for at in range(0, fs, chunk):
        rows = slice(at * capacity, (at + chunk) * capacity)
        far_rows = compact(far_tokens[at : at + chunk], pick[at : at + chunk])

        def project(mine):
            total = 0.0
            for step, piece in enumerate(near_rows):
                first = ((my_tp - step) % tp) * near_share
                block = lax.dynamic_slice_in_dim(mine, first, near_share, 0)
                total = total + jnp.dot(piece[rows], block, preferred_element_type=jnp.float32)
            return total + jnp.dot(far_rows, mine[near:], preferred_element_type=jnp.float32)

        gate_pre = jnp.minimum(project(gate_mine), LIMIT)
        up_pre = jnp.clip(project(up_mine), -LIMIT, LIMIT)
        hidden = ((up_pre + 1.0) * gate_pre * jax.nn.sigmoid(ALPHA * gate_pre)).astype(jnp.bfloat16)
        outs.append(ring_pieces(lambda step: hidden, "tp"))
    summed = []
    for pieces in outs:
        total = 0.0
        for step, cols in enumerate(pieces):
            total = total + jnp.dot(cols, down_block(-step), preferred_element_type=jnp.float32)
        summed.append(total.astype(jnp.bfloat16).reshape(chunk, capacity, out_cols))
    summed = jnp.concatenate(summed, axis=0)
    back = jnp.einsum("sct,scd->std", pick, summed, preferred_element_type=jnp.float32)
    back = (back * weight[:, :, None]).astype(jnp.bfloat16).reshape(fs * tok_rows, out_cols)
    mixed = lax.psum_scatter(back, "fs", scatter_dimension=0, tiled=True)
    return (gate_mine[None], up_mine[None], down_mine[None], mixed)


def solution(mesh):
    return jax.shard_map(
        shards,
        mesh=mesh,
        in_specs=(
            P(("grp", "fs"), None),
            P(("grp", "fs"), None),
            P(("grp", "fs"), None),
            P("fs"),
            P(None, "fs", "tp"),
            P(None, "fs", "tp"),
            P(None, "fs", "tp"),
        ),
        out_specs=(
            P(("grp", "fs"), None, "tp"),
            P(("grp", "fs"), None, "tp"),
            P(("grp", "fs"), "tp", None),
            P(("grp", "fs"), "tp"),
        ),
        check_vma=False,
    )
```
